32 devices in a mesh: kv: 8 (over z, y), tp: 4 (over x, core).
Axes of the slice: x: 2, y: 2, z: 4, core: 2. Of those that a mesh axis runs over, the one named last changes fastest.
Arguments:
- tokens: bfloat16 [16, 4, 4096], P(None, None, 'kv'), may hold values from -20 to 20
- mix_gain: float32 [4096], P('kv'), may hold values from 0.1 to 1.9
- w_query: bfloat16 [4096, 2048], P('kv', 'tp'), may hold values from -0.09375 to 0.09375
- w_key: bfloat16 [4096, 2048], P('kv', 'tp'), may hold values from -0.09375 to 0.09375
- w_value: bfloat16 [4096, 2048], P('kv', 'tp'), may hold values from -0.09375 to 0.09375
- w_forget: bfloat16 [4096, 16], replicated, may hold values from -0.09375 to 0.09375
- forget_bias: float32 [16], P('tp'), may hold values from -1 to 3
- key_cache: bfloat16 [16, 4096, 2048], P(None, 'kv', 'tp'), may hold values from -6 to 6
- value_cache: bfloat16 [16, 4096, 2048], P(None, 'kv', 'tp'), may hold values from -6 to 6
- cum_gate: float32 [16, 16, 4096], P(None, 'tp', 'kv'), may hold values from -761.52 to 0, as said below
- lengths: int32 [16], replicated, may hold values from 1 to 4096, 16381 in all
- w_out: bfloat16 [2048, 4096], P('tp', 'kv'), may hold values from -0.125 to 0.125
- mlp_gain: float32 [4096], P('kv'), may hold values from 0.1 to 1.9
- w_gate: bfloat16 [4096, 11264], P('kv', 'tp'), may hold values from -0.09375 to 0.09375
- w_up: bfloat16 [4096, 11264], P('kv', 'tp'), may hold values from -0.09375 to 0.09375
- w_down: bfloat16 [11264, 4096], P('tp', 'kv'), may hold values from -0.0546875 to 0.0546875
Outputs:
- result: bfloat16 [16, 4, 4096], P(None, None, 'kv')
The draws below stay inside these ranges and needn't reach their ends.
Inputs may be any that keep to these rules, and one draw needn't show every extreme that they name: `cum_gate`: never rising along positions. `lengths`: one sequence fills all 4096 positions.
All inputs are finite; a program needn't handle non-finite values.
Results may differ from the reference program's by a relative error of at most 0.02.
Values may be sent and summed in bfloat16 or wider, within the bound.
A program may use at most 64 MiB of HBM per device.

```python
import math
import jax
import jax.numpy as jnp
import numpy as np
from jax import lax

D = 4096
ATTENTION_HEADS = 16
HEAD_DIM = 128
FF = 11264
NEW = 4
SEQUENCE_COUNT = 16
POS_DEV = 512
CACHE_SLOTS = 4096
N_KV = 8
N_TP = 4


def draw_tokens(key, part):
    base_key, scale_key = jax.random.split(jax.random.fold_in(key, 11))
    values = jax.random.normal(base_key, (SEQUENCE_COUNT, NEW, D), jnp.float32)
    column = jnp.arange(D, dtype=jnp.float32) / D
    jaggedness = jax.random.uniform(scale_key, (D,), jnp.float32, 0.6, 1.4)
    col_scale = 3.0 ** column * jaggedness * 0.6
    return jnp.clip(values * col_scale, -20.0, 20.0).astype(jnp.bfloat16)


def draw_cum_gate(key, part):
    random_subkeys = jax.random.split(jax.random.fold_in(key, 23), 8)
    head_order = jax.random.permutation(random_subkeys[0], ATTENTION_HEADS)
    sluggish_heads = head_order >= ATTENTION_HEADS // 2
    fast_rate = jax.random.uniform(random_subkeys[1], (SEQUENCE_COUNT, ATTENTION_HEADS, 1), jnp.float32, 1.0 / 60.0, 1.0 / 30.0)
    slow_rate = jax.random.uniform(random_subkeys[2], (SEQUENCE_COUNT, ATTENTION_HEADS, 1), jnp.float32, 0.5, 1.5) / CACHE_SLOTS
    forget_speed = jnp.where(sluggish_heads[None, :, None], slow_rate, fast_rate)
    block_count = CACHE_SLOTS // POS_DEV
    block_multiplier = jnp.exp(jax.random.uniform(random_subkeys[3], (SEQUENCE_COUNT, ATTENTION_HEADS, block_count, 1), jnp.float32, -0.7, 0.7))
    block_multiplier = jnp.broadcast_to(block_multiplier, (SEQUENCE_COUNT, ATTENTION_HEADS, block_count, POS_DEV)).reshape(SEQUENCE_COUNT, ATTENTION_HEADS, CACHE_SLOTS)
    jaggedness = jax.random.uniform(random_subkeys[4], (SEQUENCE_COUNT, ATTENTION_HEADS, CACHE_SLOTS), jnp.float32, 0.3, 1.7)
    sudden_mask = jax.random.uniform(random_subkeys[5], (SEQUENCE_COUNT, ATTENTION_HEADS, CACHE_SLOTS), jnp.float32) < 4.0 / CACHE_SLOTS
    sudden_dropout = jax.random.uniform(random_subkeys[6], (SEQUENCE_COUNT, ATTENTION_HEADS, CACHE_SLOTS), jnp.float32, 0.22, 0.69)
    sudden_dropout = jnp.where(sudden_mask & sluggish_heads[None, :, None], sudden_dropout, 0.0)
    history_start = -jax.random.uniform(random_subkeys[7], (SEQUENCE_COUNT, ATTENTION_HEADS, 1), jnp.float32, 20.0, 260.0)
    gate_logarithms = -forget_speed * block_multiplier * jaggedness - sudden_dropout
    return (history_start + jnp.cumsum(gate_logarithms, axis=2)).astype(jnp.float32)


def block_scale(own_key, dims, cuts, low, largest):
    def one(dim, shards_of):
        heights = jax.random.uniform(jax.random.fold_in(jax.random.fold_in(own_key, 6), dim), (shards_of,), jnp.float32, low / len(cuts), largest / len(cuts))
        return jnp.repeat(jnp.exp(heights), dims[dim] // shards_of).reshape((-1,) + (1,) * (len(dims) - dim - 1))

    gain = one(*cuts[0])
    for cut in cuts[1:]:
        gain = gain * one(*cut)
    return gain


def profile(amount, total, bound, skew):
    loads = [(1 << 20) // math.isqrt(standing ** skew) + 1 for standing in range(2, amount + 1)]
    surplus, given = total - bound - (amount - 1), [1] * (amount - 1)
    while surplus > 0:
        candidates = [i for i in range(amount - 1) if given[i] < bound]
        pool, budget = sum([loads[i] for i in candidates]), surplus
        for i in candidates:
            addition = min(bound - given[i], max(1, budget * loads[i] // pool), surplus)
            given[i] = given[i] + addition
            surplus = surplus - addition
    return np.array([bound] + given)


def uneven(rng, count, total, reach, lean):
    if count == 2:
        one = jax.random.randint(rng, (), max(1, total - reach), min(reach, total - 1) + 1)
        return jnp.stack([one, total - one])
    sizes = jnp.asarray(profile(count, total, reach, lean), jnp.int32)
    pairs = (count - 1) // 2
    source_of, taker = sizes[1:1 + 2 * pairs:2], sizes[2:2 + 2 * pairs:2]
    slack = jnp.minimum(source_of - 1, reach - taker)
    passed = jax.random.randint(jax.random.fold_in(rng, 1), (pairs,), 0, 1 << 20) % (slack + 1)
    sizes = sizes.at[1:1 + 2 * pairs:2].set(source_of - passed).at[2:2 + 2 * pairs:2].set(taker + passed)
    return sizes[jax.random.permutation(jax.random.fold_in(rng, 2), count)]


def gaussian(rng, shape, deviation, bound, cuts=(), kind=jnp.bfloat16):
    array = deviation * jax.random.normal(rng, shape, jnp.float32)
    if cuts:
        array = array * block_scale(rng, shape, cuts, -0.22, 0.18)
    return jnp.clip(array, -bound, bound).astype(kind)


def setup_inputs(seed: int = 0) -> dict:
    key_of = jax.random.split(jax.random.key(seed), 17)
    tokens = draw_tokens(jax.random.fold_in(key_of[16], 71), 0)
    mix_gain = jnp.clip(1.0 + 0.18 * jax.random.normal(key_of[1], (D,), jnp.float32), 0.1, 1.9)
    w_query = gaussian(key_of[2], (D, ATTENTION_HEADS * HEAD_DIM), D ** -0.5, 0.09375, ((0, 8), (1, 4)))
    w_key = gaussian(key_of[3], (D, ATTENTION_HEADS * HEAD_DIM), D ** -0.5, 0.09375, ((0, 8), (1, 4)))
    w_value = gaussian(key_of[4], (D, ATTENTION_HEADS * HEAD_DIM), D ** -0.5, 0.09375, ((0, 8), (1, 4)))
    w_forget = gaussian(key_of[5], (D, ATTENTION_HEADS), D ** -0.5, 0.09375)
    forget_bias = jnp.clip(-1.0 + 4.0 * jax.random.uniform(key_of[6], (ATTENTION_HEADS,), jnp.float32) ** block_scale(key_of[6], (ATTENTION_HEADS,), ((0, 4),), -0.2, 0.2), -1.0, 3.0)
    key_cache = gaussian(key_of[7], (SEQUENCE_COUNT, CACHE_SLOTS, ATTENTION_HEADS * HEAD_DIM), 1.0, 6.0, ((1, 8), (2, 4)))
    value_cache = gaussian(key_of[8], (SEQUENCE_COUNT, CACHE_SLOTS, ATTENTION_HEADS * HEAD_DIM), 1.0, 6.0, ((1, 8), (2, 4)))
    cum_gate = draw_cum_gate(jax.random.fold_in(key_of[16], 71), 0)
    lengths = uneven(key_of[10], SEQUENCE_COUNT, CACHE_SLOTS + (SEQUENCE_COUNT - 1) * (CACHE_SLOTS // 5), CACHE_SLOTS, 2).astype(jnp.int32)
    w_out = gaussian(key_of[11], (ATTENTION_HEADS * HEAD_DIM, D), (ATTENTION_HEADS * HEAD_DIM) ** -0.5, 0.125, ((0, 4), (1, 8)))
    mlp_gain = jnp.clip(1.0 + 0.18 * jax.random.normal(key_of[12], (D,), jnp.float32), 0.1, 1.9)
    w_gate = gaussian(key_of[13], (D, FF), D ** -0.5, 0.09375, ((0, 8), (1, 4)))
    w_up = gaussian(key_of[14], (D, FF), D ** -0.5, 0.09375, ((0, 8), (1, 4)))
    w_down = gaussian(key_of[15], (FF, D), FF ** -0.5, 0.0546875, ((0, 4), (1, 8)))
    return dict(tokens=tokens, mix_gain=mix_gain, w_query=w_query, w_key=w_key, w_value=w_value, w_forget=w_forget, forget_bias=forget_bias, key_cache=key_cache, value_cache=value_cache, cum_gate=cum_gate, lengths=lengths, w_out=w_out, mlp_gain=mlp_gain, w_gate=w_gate, w_up=w_up, w_down=w_down)


EPSILON = 1e-06
NEG_FILL = -1e+30

def widen(values):
    return lax.optimization_barrier(values).astype(jnp.float32)

def grouped_sum(left, weight, group_width):
    summed = jnp.zeros((left.shape[0], weight.shape[1]), jnp.float32)
    for group in range(N_TP):
        partial_product = jnp.dot(left[:, group * group_width:(group + 1) * group_width], weight[group * group_width:(group + 1) * group_width], preferred_element_type=jnp.float32)
        summed = summed + widen(partial_product.astype(jnp.bfloat16))
    return summed

def reference(tokens, mix_gain, w_query, w_key, w_value, w_forget, forget_bias, key_cache, value_cache, cum_gate, lengths, w_out, mlp_gain, w_gate, w_up, w_down):
    row_count = SEQUENCE_COUNT * NEW
    inputs = tokens.reshape(row_count, D).astype(jnp.float32)
    inv_norm = lax.rsqrt(lax.optimization_barrier(jnp.sum(inputs * inputs, axis=1)) / D + EPSILON)[:, None]
    scaled = (inputs * mix_gain).astype(jnp.bfloat16)

    def project(weight):
        return inv_norm * jnp.dot(scaled, weight, preferred_element_type=jnp.float32)
    query = project(w_query).astype(jnp.bfloat16).reshape(SEQUENCE_COUNT, NEW, ATTENTION_HEADS, HEAD_DIM)
    key_new = project(w_key).astype(jnp.bfloat16).reshape(SEQUENCE_COUNT, NEW, ATTENTION_HEADS, HEAD_DIM)
    value_new = project(w_value).astype(jnp.bfloat16).reshape(SEQUENCE_COUNT, NEW, ATTENTION_HEADS, HEAD_DIM)
    log_forget = jax.nn.log_sigmoid(project(w_forget) + forget_bias).reshape(SEQUENCE_COUNT, NEW, ATTENTION_HEADS)
    score_scale = HEAD_DIM ** (-0.5)
    query_wide = widen(query)

    def past_block(block_index):
        offset = block_index * POS_DEV
        cached_keys = lax.dynamic_slice_in_dim(key_cache, offset, POS_DEV, 1).astype(jnp.float32)
        cached_keys = cached_keys.reshape(SEQUENCE_COUNT, POS_DEV, ATTENTION_HEADS, HEAD_DIM)
        cached_values = lax.dynamic_slice_in_dim(value_cache, offset, POS_DEV, 1).astype(jnp.float32)
        cached_values = cached_values.reshape(SEQUENCE_COUNT, POS_DEV, ATTENTION_HEADS, HEAD_DIM)
        cum_block = lax.dynamic_slice_in_dim(cum_gate, offset, POS_DEV, 2)
        scores = jnp.einsum('bthd,bphd->bthp', query_wide, cached_keys) * score_scale - cum_block[:, None]
        positions = offset + jnp.arange(POS_DEV, dtype=jnp.int32)
        live_mask = (positions[None, :] < lengths[:, None])[:, None, None, :]
        scores = jnp.where(live_mask, scores, NEG_FILL)
        block_peak = lax.optimization_barrier(jnp.max(scores, axis=3))
        weights = jnp.where(live_mask, jnp.exp(scores - block_peak[..., None]), 0.0)
        block_total = lax.optimization_barrier(jnp.sum(weights, axis=3))
        block_sum = jnp.einsum('bthp,bphd->bthd', widen(weights.astype(jnp.bfloat16)), cached_values)
        return (block_peak, block_total, block_sum)
    peaks, totals, sums = lax.map(past_block, jnp.arange(N_KV, dtype=jnp.int32))
    past_peak = lax.optimization_barrier(jnp.max(peaks, axis=0))
    factors = jnp.exp(peaks - past_peak)
    past_total = lax.optimization_barrier(jnp.sum(totals * factors, axis=0))
    past_sum = lax.optimization_barrier(jnp.sum(sums * factors[..., None], axis=0))
    last_index = jnp.broadcast_to((lengths - 1).astype(jnp.int32)[:, None, None], (SEQUENCE_COUNT, ATTENTION_HEADS, 1))
    last_cum = jnp.take_along_axis(cum_gate, last_index, axis=2)[..., 0]
    key_cum = last_cum[:, None, :] + jnp.cumsum(log_forget, axis=1)
    own_scores = jnp.einsum('bthd,bshd->bths', query_wide, widen(key_new)) * score_scale
    own_scores = own_scores - jnp.transpose(key_cum, (0, 2, 1))[:, None]
    causal = (jnp.arange(NEW)[:, None] >= jnp.arange(NEW)[None, :])[None, :, None, :]
    own_scores = jnp.where(causal, own_scores, NEG_FILL)
    peak_score = jnp.maximum(past_peak, lax.optimization_barrier(jnp.max(own_scores, axis=3)))
    past_factor = jnp.exp(past_peak - peak_score)
    own_weights = jnp.where(causal, jnp.exp(own_scores - peak_score[..., None]), 0.0)
    numerator = past_sum * past_factor[..., None] + jnp.einsum('bths,bshd->bthd', widen(own_weights.astype(jnp.bfloat16)), widen(value_new))
    denominator = past_total * past_factor + lax.optimization_barrier(jnp.sum(own_weights, axis=3))
    attended = (numerator / denominator[..., None]).astype(jnp.bfloat16).reshape(row_count, ATTENTION_HEADS * HEAD_DIM)
    attn_out = grouped_sum(attended, w_out, ATTENTION_HEADS // N_TP * HEAD_DIM)
    middle = (inputs + attn_out).astype(jnp.bfloat16)
    middle_wide = middle.astype(jnp.float32)
    inv_norm2 = lax.rsqrt(lax.optimization_barrier(jnp.sum(middle_wide * middle_wide, axis=1)) / D + EPSILON)[:, None]
    scaled2 = (middle_wide * mlp_gain).astype(jnp.bfloat16)
    gate = inv_norm2 * jnp.dot(scaled2, w_gate, preferred_element_type=jnp.float32)
    up_proj = inv_norm2 * jnp.dot(scaled2, w_up, preferred_element_type=jnp.float32)
    hidden = (jax.nn.silu(gate) * up_proj).astype(jnp.bfloat16)
    mixed = grouped_sum(hidden, w_down, FF // N_TP)
    return (middle_wide + mixed).astype(jnp.bfloat16).reshape(SEQUENCE_COUNT, NEW, D)
```

```python
import jax
import jax.numpy as jnp
import functools

from jax import lax
from jax.experimental import pallas as pl
from jax.experimental.pallas import tpu as pltpu
from jax.sharding import PartitionSpec as P

EPSILON = 1e-06
NEG_FILL = -1e30


def combined_all(array, axis, combine):
    everything = jax.tree.map(lambda part: lax.all_gather(part, axis), array)
    first = jax.tree.map(lambda part: part[0], everything)

    def turn(k, so_far):
        return combine(so_far, jax.tree.map(lambda part: part[k], everything))

    return lax.fori_loop(1, lax.axis_size(axis), turn, first)


def on_device(
    tokens,
    mix_gain,
    w_query,
    w_key,
    w_value,
    w_forget,
    forget_bias,
    key_cache,
    value_cache,
    cum_gate,
    lengths,
    w_out,
    mlp_gain,
    w_gate,
    w_up,
    w_down,
):
    seq_count, new_count, local_width = tokens.shape
    D = local_width * lax.axis_size("kv")
    row_count = seq_count * new_count
    heads_dev = forget_bias.shape[0]
    head_width = w_query.shape[1] // heads_dev
    pos_dev = key_cache.shape[1]
    kv_index = lax.axis_index("kv")
    tp_index = lax.axis_index("tp")
    inputs = tokens.reshape(row_count, local_width).astype(jnp.float32)
    scaled = (inputs * mix_gain).astype(jnp.bfloat16)
    forget_rows = lax.dynamic_slice_in_dim(w_forget, kv_index * local_width, local_width, 0)
    forget_cols = lax.dynamic_slice_in_dim(forget_rows, tp_index * heads_dev, heads_dev, 1)
    query_part = jnp.dot(scaled, w_query, preferred_element_type=jnp.float32)
    key_part = jnp.dot(scaled, w_key, preferred_element_type=jnp.float32)
    value_part = jnp.dot(scaled, w_value, preferred_element_type=jnp.float32)
    forget_part = jnp.dot(scaled, forget_cols, preferred_element_type=jnp.float32)
    squares = jnp.sum(inputs * inputs, axis=1)
    query_sum, key_sum, value_sum, forget_sum, square_sum = (
        lax.psum(query_part.astype(jnp.bfloat16), "kv").astype(jnp.float32),
        lax.psum(key_part.astype(jnp.bfloat16), "kv").astype(jnp.float32),
        lax.psum(value_part.astype(jnp.bfloat16), "kv").astype(jnp.float32),
        lax.psum(forget_part.astype(jnp.bfloat16), "kv").astype(jnp.float32),
        lax.psum(squares.astype(jnp.bfloat16), "kv").astype(jnp.float32),
    )
    inv_norm = lax.rsqrt(square_sum / D + EPSILON)[:, None]
    head_shape = (seq_count, new_count, heads_dev, head_width)
    query = (inv_norm * query_sum).astype(jnp.bfloat16).reshape(head_shape)
    key_new = (inv_norm * key_sum).astype(jnp.bfloat16).reshape(head_shape)
    value_new = (inv_norm * value_sum).astype(jnp.bfloat16).reshape(head_shape)
    log_forget = jax.nn.log_sigmoid(inv_norm * forget_sum + forget_bias).reshape(
        seq_count, new_count, heads_dev
    )
    score_scale = head_width ** (-0.5)
    positions = kv_index * pos_dev + jnp.arange(pos_dev, dtype=jnp.int32)
    live_rows = positions[None, :] < lengths[:, None]
    live_mask = live_rows[:, None, None, :]
    cached_keys = key_cache.reshape(seq_count, pos_dev, heads_dev, head_width)
    cached_values = value_cache.reshape(seq_count, pos_dev, heads_dev, head_width)
    scores = jnp.einsum("bthd,bphd->bthp", query, cached_keys, preferred_element_type=jnp.float32)
    scores = scores * score_scale - cum_gate[:, None]
    scores = jnp.where(live_mask, scores, NEG_FILL)
    block_peak = jnp.max(scores, axis=3)
    weights = jnp.where(live_mask, jnp.exp(scores - block_peak[..., None]), 0.0)
    block_total = jnp.sum(weights, axis=3)
    block_sum = jnp.einsum(
        "bthp,bphd->bthd",
        weights.astype(jnp.bfloat16),
        cached_values,
        preferred_element_type=jnp.float32,
    )
    last_hit = positions[None, :] == (lengths - 1)[:, None]
    last_piece = jnp.sum(jnp.where(last_hit[:, None, :], cum_gate, 0.0), axis=2)

    def combine(first, second):
        peak_both = jnp.maximum(first[0], second[0])
        first_factor = jnp.exp(first[0] - peak_both)
        second_factor = jnp.exp(second[0] - peak_both)
        return (
            peak_both,
            first[1] * first_factor + second[1] * second_factor,
            first[2] * first_factor[..., None] + second[2] * second_factor[..., None],
            first[3] + second[3],
        )

    past_peak, past_total, past_sum, last_cum = combined_all(
        (block_peak, block_total, block_sum, last_piece), "kv", combine
    )
    key_cum = last_cum[:, None, :] + jnp.cumsum(log_forget, axis=1)
    own_scores = (
        jnp.einsum("bthd,bshd->bths", query, key_new, preferred_element_type=jnp.float32)
        * score_scale
    )
    own_scores = own_scores - jnp.transpose(key_cum, (0, 2, 1))[:, None]
    causal = (jnp.arange(new_count)[:, None] >= jnp.arange(new_count)[None, :])[None, :, None, :]
    own_scores = jnp.where(causal, own_scores, NEG_FILL)
    peak_score = jnp.maximum(past_peak, jnp.max(own_scores, axis=3))
    past_factor = jnp.exp(past_peak - peak_score)
    own_weights = jnp.where(causal, jnp.exp(own_scores - peak_score[..., None]), 0.0)
    numerator = past_sum * past_factor[..., None] + jnp.einsum(
        "bths,bshd->bthd",
        own_weights.astype(jnp.bfloat16),
        value_new,
        preferred_element_type=jnp.float32,
    )
    denominator = past_total * past_factor + jnp.sum(own_weights, axis=3)
    attended = (
        (numerator / denominator[..., None])
        .astype(jnp.bfloat16)
        .reshape(row_count, heads_dev * head_width)
    )
    attn_out = lax.psum(
        jnp.dot(attended, w_out, preferred_element_type=jnp.float32).astype(jnp.bfloat16), "tp"
    ).astype(jnp.float32)
    middle = (inputs + attn_out).astype(jnp.bfloat16)
    middle_wide = middle.astype(jnp.float32)
    squares2 = jnp.sum(middle_wide * middle_wide, axis=1)
    scaled2 = (middle_wide * mlp_gain).astype(jnp.bfloat16)
    gate_part = jnp.dot(scaled2, w_gate, preferred_element_type=jnp.float32)
    up_part = jnp.dot(scaled2, w_up, preferred_element_type=jnp.float32)
    gate_sum, up_sum, square_sum2 = (
        lax.psum(gate_part.astype(jnp.bfloat16), "kv").astype(jnp.float32),
        lax.psum(up_part.astype(jnp.bfloat16), "kv").astype(jnp.float32),
        lax.psum(squares2.astype(jnp.bfloat16), "kv").astype(jnp.float32),
    )
    inv_norm2 = lax.rsqrt(square_sum2 / D + EPSILON)[:, None]
    hidden = (jax.nn.silu(inv_norm2 * gate_sum) * (inv_norm2 * up_sum)).astype(jnp.bfloat16)
    down_part = jnp.dot(hidden, w_down, preferred_element_type=jnp.float32)
    mixed = lax.psum(down_part.astype(jnp.bfloat16), "tp").astype(jnp.float32)
    return (middle_wide + mixed).astype(jnp.bfloat16).reshape(seq_count, new_count, local_width)


LANES = 128
MESH = pl.DeviceIdType.MESH
F32 = jnp.float32
BF16 = jnp.bfloat16


def fused_kernel(
    n_kv, n_tp, new_count,
    tok, mix_gain, mlp_gain, bias, lens, wf_h, cum_h, wq_h, wk_h, wv_h,
    kc_h, vc_h, wo_h, wg_h, wu_h, wd_h,
    out,
    wf, cum, wq, wk, wv, kc, vc, wo, wg, wu, wd,
    sb1, rb1, qb, kn, vn, lf, cs, cr, ab, ap, ar, mid, gs, gr, us, ur, hb, dp, dr,
    lsem, ksem, vsem, s1, r1, s2, r2, s3, r3, s4, r4, s5, r5, s6, r6, s7, r7, s8, r8, s9, r9,
):
    me = lax.axis_index("kv")
    mt = lax.axis_index("tp")
    rows, width = tok.shape
    rp = rows // n_kv
    sp = rp // new_count
    heads = bias.shape[0]
    hw = wq.shape[1]
    hd = hw // heads
    pos_dev = kc.shape[1]
    ff = wg.shape[1]
    full = width * n_kv
    scale = hd ** (-0.5)

    def peer(i):
        return lax.rem(me + i, n_kv)

    def tpeer(i):
        return lax.rem(mt + i, n_tp)

    loads = [
        pltpu.make_async_copy(wf_h.at[pl.ds(pl.multiple_of(me * width, width), width)], wf, lsem.at[0]),
        pltpu.make_async_copy(wq_h, wq, lsem.at[1]),
        pltpu.make_async_copy(wk_h, wk, lsem.at[2]),
        pltpu.make_async_copy(wv_h, wv, lsem.at[3]),
        pltpu.make_async_copy(cum_h, cum, lsem.at[4]),
        pltpu.make_async_copy(wo_h, wo, lsem.at[5]),
        pltpu.make_async_copy(wg_h, wg, lsem.at[6]),
        pltpu.make_async_copy(wu_h, wu, lsem.at[7]),
        pltpu.make_async_copy(wd_h, wd, lsem.at[8]),
    ]

    def cache_copies(g):
        part = pl.ds(g * sp, sp)
        return (
            pltpu.make_async_copy(kc_h.at[part], kc.at[part], ksem.at[g]),
            pltpu.make_async_copy(vc_h.at[part], vc.at[part], vsem.at[g]),
        )

    for load in loads[:5]:
        load.start()

    def start_cache(i, c):
        for copy in cache_copies(peer(i)):
            copy.start()
        return c

    lax.fori_loop(0, n_kv, start_cache, 0)
    for load in loads[5:]:
        load.start()

    barrier = pltpu.get_barrier_semaphore()
    for i in range(1, n_kv):
        pl.semaphore_signal(barrier, inc=1, device_id={"kv": peer(i)}, device_id_type=MESH)
    for i in range(1, n_tp):
        pl.semaphore_signal(barrier, inc=1, device_id={"tp": tpeer(i)}, device_id_type=MESH)

    def send_kv(src, dst, send, recv, g):
        return pltpu.make_async_remote_copy(
            src_ref=src, dst_ref=dst, send_sem=send, recv_sem=recv,
            device_id={"kv": g}, device_id_type=MESH,
        )

    def send_tp(src, dst, send, recv, g):
        return pltpu.make_async_remote_copy(
            src_ref=src, dst_ref=dst, send_sem=send, recv_sem=recv,
            device_id={"tp": g}, device_id_type=MESH,
        )

    inputs = tok[...].astype(F32)
    scaled = (inputs * mix_gain[...]).astype(BF16)
    squares = jnp.sum(inputs * inputs, axis=1, keepdims=True)
    loads[0].wait()
    forget_all = jnp.dot(scaled, wf[...], preferred_element_type=F32).astype(BF16)
    pick_row = lax.broadcasted_iota(jnp.int32, (wf.shape[1], LANES), 0)
    pick_col = lax.broadcasted_iota(jnp.int32, (wf.shape[1], LANES), 1)
    pick = jnp.where(
        (pick_row == pick_col + mt * heads) & (pick_col < heads), 1.0, 0.0
    ).astype(BF16)
    forget = jnp.dot(forget_all, pick, preferred_element_type=F32)
    lane_rows = lax.broadcasted_iota(jnp.int32, (rows, LANES), 1)
    aux = jnp.where(lane_rows == heads, squares, forget)
    for g in range(n_kv):
        sb1[g, :, 3 * hw :] = aux[g * rp : (g + 1) * rp].astype(BF16)
    for k, (load, weight) in enumerate(zip(loads[1:4], (wq, wk, wv))):
        load.wait()
        part = jnp.dot(scaled, weight[...], preferred_element_type=F32)
        for g in range(n_kv):
            sb1[g, :, k * hw : (k + 1) * hw] = part[g * rp : (g + 1) * rp].astype(BF16)

    pl.semaphore_wait(barrier, n_kv + n_tp - 2)
    for i in range(1, n_kv):
        g = peer(i)
        send_kv(sb1.at[g], rb1.at[me], s1.at[g], r1.at[me], g).start()
    total1 = sb1[me].astype(F32)
    for i in range(1, n_kv):
        g = peer(i)
        send_kv(sb1.at[g], rb1.at[g], s1.at[g], r1.at[g], g).wait_recv()
        total1 = total1 + rb1[g].astype(F32)
    lane = lax.broadcasted_iota(jnp.int32, (rp, LANES), 1)
    row8 = lax.broadcasted_iota(jnp.int32, (rp, LANES), 0)
    aux1 = total1[:, 3 * hw :]
    inv_norm = lax.rsqrt(aux1[:, heads : heads + 1] / full + EPSILON)
    qb[me] = (inv_norm * total1[:, :hw]).astype(BF16)
    for i in range(1, n_kv):
        g = peer(i)
        send_kv(qb.at[me], qb.at[me], s2.at[g], r2.at[me], g).start()
    kn[...] = (inv_norm * total1[:, hw : 2 * hw]).astype(BF16).astype(F32)
    vn[...] = (inv_norm * total1[:, 2 * hw : 3 * hw]).astype(BF16).astype(F32)
    bias_row = jnp.zeros((rp, LANES), F32)
    for h in range(heads):
        bias_row = jnp.where(lane == h, bias[h], bias_row)
    logit = inv_norm * aux1 + bias_row
    lf[...] = -(jnp.maximum(-logit, 0.0) + jnp.log1p(jnp.exp(-jnp.abs(logit))))

    loads[4].wait()
    col_q = lax.broadcasted_iota(jnp.int32, (rp, hw), 1)
    row_p = lax.broadcasted_iota(jnp.int32, (rp, pos_dev), 0)
    pos = me * pos_dev + lax.broadcasted_iota(jnp.int32, (rp, pos_dev), 1)

    def attend(g, dest):
        q8 = qb[g].astype(F32)
        spread = jnp.concatenate(
            [
                jnp.where((col_q >= h * hd) & (col_q < (h + 1) * hd), q8, 0.0)
                for h in range(heads)
            ],
            axis=0,
        ).astype(BF16)
        copy_k, copy_v = cache_copies(g)
        copy_k.wait()
        length = jnp.zeros((rp, pos_dev), jnp.int32)
        products, gates = [], []
        for j in range(sp):
            products.append(
                lax.dot_general(
                    spread, kc[g * sp + j], (((1,), (1,)), ((), ())), preferred_element_type=F32
                )
            )
            gates.append(cum[g * sp + j])
            length = jnp.where(row_p >= j * new_count, lens[g * sp + j], length)
        live = pos < length
        last_hit = pos == length - 1
        weight_heads = []
        extra = jnp.zeros((rp, LANES), F32)
        for h in range(heads):
            score, gate = None, None
            for j in range(sp):
                score_j = products[j][h * rp : (h + 1) * rp]
                gate_j = jnp.broadcast_to(gates[j][h : h + 1], (rp, pos_dev))
                if j == 0:
                    score, gate = score_j, gate_j
                else:
                    score = jnp.where(row_p >= j * new_count, score_j, score)
                    gate = jnp.where(row_p >= j * new_count, gate_j, gate)
            score = jnp.where(live, score * scale - gate, NEG_FILL)
            peak = jnp.max(score, axis=1, keepdims=True)
            weight = jnp.where(live, jnp.exp(score - peak), 0.0)
            extra = jnp.where(lane == h, peak, extra)
            extra = jnp.where(lane == heads + h, jnp.sum(weight, axis=1, keepdims=True), extra)
            last = jnp.sum(jnp.where(last_hit, gate, 0.0), axis=1, keepdims=True)
            extra = jnp.where(lane == 2 * heads + h, last, extra)
            weight_heads.append(weight)
        weights = jnp.concatenate(weight_heads, axis=0).astype(BF16)
        copy_v.wait()
        sums = [
            jnp.dot(weights, vc[g * sp + j], preferred_element_type=F32) for j in range(sp)
        ]
        row_h = row8[:, :1]
        for h in range(heads):
            piece = sums[0][h * rp : (h + 1) * rp, h * hd : (h + 1) * hd]
            for j in range(1, sp):
                piece_j = sums[j][h * rp : (h + 1) * rp, h * hd : (h + 1) * hd]
                piece = jnp.where(row_h >= j * new_count, piece_j, piece)
            dest[:, h * hd : (h + 1) * hd] = piece
        dest[:, hw:] = extra

    attend(me, cr.at[me])

    def attend_step(i, c):
        g = peer(i)
        send_kv(qb.at[me], qb.at[g], s2.at[g], r2.at[g], g).wait_recv()
        attend(g, cs.at[g])
        send_kv(cs.at[g], cr.at[me], s3.at[g], r3.at[me], g).start()
        return c

    lax.fori_loop(1, n_kv, attend_step, 0)

    for i in range(1, n_kv):
        g = peer(i)
        send_kv(cs.at[g], cr.at[g], s3.at[g], r3.at[g], g).wait_recv()

    def expand(x):
        return jnp.concatenate(
            [jnp.broadcast_to(x[:, h : h + 1], (rp, hd)) for h in range(heads)], axis=1
        )

    extras = [cr[k, :, hw:] for k in range(n_kv)]
    past_peak = functools.reduce(jnp.maximum, extras)
    past_total = jnp.zeros((rp, LANES), F32)
    last_cum = jnp.zeros((rp, LANES), F32)
    past_sum = jnp.zeros((rp, hw), F32)
    for k in range(n_kv):
        factor = jnp.exp(extras[k] - past_peak)
        past_total = past_total + pltpu.roll(extras[k], LANES - heads, 1) * factor
        last_cum = last_cum + pltpu.roll(extras[k], LANES - 2 * heads, 1)
        past_sum = past_sum + cr[k, :, :hw] * expand(factor)

    def valid(d):
        hit = (row8 >= d) & (row8 < new_count)
        for j in range(1, sp):
            hit = hit | ((row8 >= j * new_count + d) & (row8 < (j + 1) * new_count))
        return hit

    def shifted(x, d):
        return x if d == 0 else pltpu.roll(x, d, 0)

    log_forget = lf[...]
    key_cum = last_cum
    for d in range(new_count):
        key_cum = key_cum + jnp.where(valid(d), shifted(log_forget, d), 0.0)
    own_query = qb[me].astype(F32)
    own_key, own_value = kn[...], vn[...]
    own_scores = []
    for d in range(new_count):
        product = own_query * shifted(own_key, d)
        score = jnp.zeros((rp, LANES), F32)
        for h in range(heads):
            dot_h = jnp.sum(product[:, h * hd : (h + 1) * hd], axis=1, keepdims=True)
            score = jnp.where(lane == h, dot_h, score)
        own_scores.append(
            jnp.where(valid(d), score * scale - shifted(key_cum, d), NEG_FILL)
        )
    peak_score = functools.reduce(jnp.maximum, own_scores, past_peak)
    past_factor = jnp.exp(past_peak - peak_score)
    numerator = past_sum * expand(past_factor)
    denominator = past_total * past_factor
    for d in range(new_count):
        own_weight = jnp.where(valid(d), jnp.exp(own_scores[d] - peak_score), 0.0)
        denominator = denominator + own_weight
        numerator = numerator + expand(own_weight.astype(BF16).astype(F32)) * shifted(own_value, d)
    ab[me] = (numerator / expand(denominator)).astype(BF16)
    for i in range(1, n_kv):
        g = peer(i)
        send_kv(ab.at[me], ab.at[me], s4.at[g], r4.at[me], g).start()
    for i in range(1, n_kv):
        g = peer(i)
        send_kv(ab.at[me], ab.at[g], s4.at[g], r4.at[g], g).wait_recv()

    def all_rows(ref):
        return jnp.concatenate([ref[k].astype(F32) for k in range(n_kv)], axis=0).astype(BF16)

    loads[5].wait()
    ap[...] = jnp.dot(all_rows(ab), wo[...], preferred_element_type=F32).astype(BF16)
    for i in range(1, n_tp):
        g = tpeer(i)
        send_tp(ap, ar.at[mt], s5.at[g], r5.at[mt], g).start()
    for i in range(1, n_tp):
        g = tpeer(i)
        send_tp(ap, ar.at[g], s5.at[g], r5.at[g], g).wait_recv()
    attn_out = jnp.zeros((rows, width), F32)
    for k in range(n_tp):
        attn_out = attn_out + jnp.where(mt == k, ap[...], ar[k]).astype(F32)
    middle = (tok[...].astype(F32) + attn_out).astype(BF16)
    mid[...] = middle
    wide = middle.astype(F32)
    squares2 = jnp.sum(wide * wide, axis=1, keepdims=True)
    scaled2 = (wide * mlp_gain[...]).astype(BF16)

    for g in range(n_kv):
        gs[g, :, ff:] = jnp.broadcast_to(squares2[g * rp : (g + 1) * rp], (rp, LANES)).astype(BF16)
    tile = 256 if ff % 256 == 0 else LANES
    for load, weight, sent, landed, ssem, rsem in (
        (loads[6], wg, gs, gr, s6, r6),
        (loads[7], wu, us, ur, s7, r7),
    ):
        load.wait()

        def column_tile(c, carry, weight=weight, sent=sent):
            cols = pl.ds(pl.multiple_of(c * tile, tile), tile)
            part = jnp.dot(scaled2, weight[:, cols], preferred_element_type=F32)
            for g in range(n_kv):
                sent[g, :, cols] = part[g * rp : (g + 1) * rp].astype(BF16)
            return carry

        lax.fori_loop(0, ff // tile, column_tile, 0)
        for i in range(1, n_kv):
            g = peer(i)
            send_kv(sent.at[g], landed.at[me], ssem.at[g], rsem.at[me], g).start()
    for i in range(1, n_kv):
        g = peer(i)
        send_kv(gs.at[g], gr.at[g], s6.at[g], r6.at[g], g).wait_recv()
    gate_sum = gs[me].astype(F32)
    for i in range(1, n_kv):
        gate_sum = gate_sum + gr[peer(i)].astype(F32)
    inv_norm2 = lax.rsqrt(gate_sum[:, ff : ff + 1] / full + EPSILON)
    gate = inv_norm2 * gate_sum[:, :ff]
    silu = gate / (1.0 + jnp.exp(-gate))
    for i in range(1, n_kv):
        g = peer(i)
        send_kv(us.at[g], ur.at[g], s7.at[g], r7.at[g], g).wait_recv()
    up_sum = us[me].astype(F32)
    for i in range(1, n_kv):
        up_sum = up_sum + ur[peer(i)].astype(F32)
    hb[me] = (silu * (inv_norm2 * up_sum)).astype(BF16)
    for i in range(1, n_kv):
        g = peer(i)
        send_kv(hb.at[me], hb.at[me], s8.at[g], r8.at[me], g).start()
    for i in range(1, n_kv):
        g = peer(i)
        send_kv(hb.at[me], hb.at[g], s8.at[g], r8.at[g], g).wait_recv()

    loads[8].wait()
    dp[...] = jnp.dot(all_rows(hb), wd[...], preferred_element_type=F32).astype(BF16)
    for i in range(1, n_tp):
        g = tpeer(i)
        send_tp(dp, dr.at[mt], s9.at[g], r9.at[mt], g).start()
    for i in range(1, n_tp):
        g = tpeer(i)
        send_tp(dp, dr.at[g], s9.at[g], r9.at[g], g).wait_recv()
    mixed = jnp.zeros((rows, width), F32)
    for k in range(n_tp):
        mixed = mixed + jnp.where(mt == k, dp[...], dr[k]).astype(F32)
    out[...] = (mid[...].astype(F32) + mixed).astype(BF16)

    for i in range(1, n_kv):
        g = peer(i)
        send_kv(sb1.at[g], rb1.at[me], s1.at[g], r1.at[me], g).wait_send()
        send_kv(qb.at[me], qb.at[me], s2.at[g], r2.at[me], g).wait_send()
        send_kv(cs.at[g], cr.at[me], s3.at[g], r3.at[me], g).wait_send()
        send_kv(ab.at[me], ab.at[me], s4.at[g], r4.at[me], g).wait_send()
        send_kv(gs.at[g], gr.at[me], s6.at[g], r6.at[me], g).wait_send()
        send_kv(us.at[g], ur.at[me], s7.at[g], r7.at[me], g).wait_send()
        send_kv(hb.at[me], hb.at[me], s8.at[g], r8.at[me], g).wait_send()
    for i in range(1, n_tp):
        g = tpeer(i)
        send_tp(ap, ar.at[mt], s5.at[g], r5.at[mt], g).wait_send()
        send_tp(dp, dr.at[mt], s9.at[g], r9.at[mt], g).wait_send()


def fused_on_device(
    tokens, mix_gain, w_query, w_key, w_value, w_forget, forget_bias, key_cache, value_cache,
    cum_gate, lengths, w_out, mlp_gain, w_gate, w_up, w_down,
):
    n_kv, n_tp = lax.axis_size("kv"), lax.axis_size("tp")
    seq_count, new_count, width = tokens.shape
    rows = seq_count * new_count
    rp = rows // n_kv
    hw = w_query.shape[1]
    ff = w_gate.shape[1]
    vmem = pl.BlockSpec(memory_space=pltpu.VMEM)
    smem = pl.BlockSpec(memory_space=pltpu.SMEM)
    anywhere = pl.BlockSpec(memory_space=pl.ANY)
    kv_sems = pltpu.SemaphoreType.DMA((n_kv,))
    tp_sems = pltpu.SemaphoreType.DMA((n_tp,))

    def like(x):
        return pltpu.VMEM(x.shape, x.dtype)

    result = pl.pallas_call(
        functools.partial(fused_kernel, n_kv, n_tp, new_count),
        out_shape=jax.ShapeDtypeStruct((rows, width), BF16),
        in_specs=[vmem] * 3 + [smem] * 2 + [anywhere] * 11,
        out_specs=vmem,
        scratch_shapes=[
            pltpu.VMEM((width, w_forget.shape[1]), BF16),
            like(cum_gate), like(w_query), like(w_key), like(w_value),
            like(key_cache), like(value_cache), like(w_out), like(w_gate), like(w_up),
            like(w_down),
            pltpu.VMEM((n_kv, rp, 3 * hw + LANES), BF16),
            pltpu.VMEM((n_kv, rp, 3 * hw + LANES), BF16),
            pltpu.VMEM((n_kv, rp, hw), BF16),
            pltpu.VMEM((rp, hw), F32),
            pltpu.VMEM((rp, hw), F32),
            pltpu.VMEM((rp, LANES), F32),
            pltpu.VMEM((n_kv, rp, hw + LANES), F32),
            pltpu.VMEM((n_kv, rp, hw + LANES), F32),
            pltpu.VMEM((n_kv, rp, hw), BF16),
            pltpu.VMEM((rows, width), BF16),
            pltpu.VMEM((n_tp, rows, width), BF16),
            pltpu.VMEM((rows, width), BF16),
            pltpu.VMEM((n_kv, rp, ff + LANES), BF16),
            pltpu.VMEM((n_kv, rp, ff + LANES), BF16),
            pltpu.VMEM((n_kv, rp, ff), BF16),
            pltpu.VMEM((n_kv, rp, ff), BF16),
            pltpu.VMEM((n_kv, rp, ff), BF16),
            pltpu.VMEM((rows, width), BF16),
            pltpu.VMEM((n_tp, rows, width), BF16),
            pltpu.SemaphoreType.DMA((9,)),
            kv_sems, kv_sems,
            kv_sems, kv_sems, kv_sems, kv_sems, kv_sems, kv_sems, kv_sems, kv_sems,
            tp_sems, tp_sems,
            kv_sems, kv_sems, kv_sems, kv_sems, kv_sems, kv_sems,
            tp_sems, tp_sems,
        ],
        compiler_params=pltpu.CompilerParams(
            collective_id=0, has_side_effects=True, vmem_limit_bytes=60 * 1024 * 1024
        ),
    )(
        tokens.reshape(rows, width), mix_gain.reshape(1, width), mlp_gain.reshape(1, width),
        forget_bias, lengths, w_forget, cum_gate, w_query, w_key, w_value,
        key_cache, value_cache, w_out, w_gate, w_up, w_down,
    )
    return result.reshape(seq_count, new_count, width)


def solution(mesh):
    in_specs = (
        P(None, None, "kv"),
        P("kv"),
        P("kv", "tp"),
        P("kv", "tp"),
        P("kv", "tp"),
        P(),
        P("tp"),
        P(None, "kv", "tp"),
        P(None, "kv", "tp"),
        P(None, "tp", "kv"),
        P(),
        P("tp", "kv"),
        P("kv"),
        P("kv", "tp"),
        P("kv", "tp"),
        P("tp", "kv"),
    )
    out_specs = P(None, None, "kv")

    def layer(*arrays):
        seq_count, new_count, _ = arrays[0].shape
        rows_kv, rest = divmod(seq_count * new_count, jax.lax.axis_size("kv"))
        if rest or rows_kv % 8 or rows_kv % new_count:
            return on_device(*arrays)
        return fused_on_device(*arrays)

    return jax.shard_map(
        layer, mesh=mesh, in_specs=in_specs, out_specs=out_specs, check_vma=False
    )
```

```python
import jax
import jax.numpy as jnp
import functools

from jax import lax
from jax.experimental import pallas as pl
from jax.experimental.pallas import tpu as pltpu
from jax.sharding import PartitionSpec as P

EPSILON = 1e-06
NEG_FILL = -1e30


def combined_all(array, axis, combine):
    everything = jax.tree.map(lambda part: lax.all_gather(part, axis), array)
    first = jax.tree.map(lambda part: part[0], everything)

    def turn(k, so_far):
        return combine(so_far, jax.tree.map(lambda part: part[k], everything))

    return lax.fori_loop(1, lax.axis_size(axis), turn, first)


def on_device(
    tokens,
    mix_gain,
    w_query,
    w_key,
    w_value,
    w_forget,
    forget_bias,
    key_cache,
    value_cache,
    cum_gate,
    lengths,
    w_out,
    mlp_gain,
    w_gate,
    w_up,
    w_down,
):
    seq_count, new_count, local_width = tokens.shape
    D = local_width * lax.axis_size("kv")
    row_count = seq_count * new_count
    heads_dev = forget_bias.shape[0]
    head_width = w_query.shape[1] // heads_dev
    pos_dev = key_cache.shape[1]
    kv_index = lax.axis_index("kv")
    tp_index = lax.axis_index("tp")
    inputs = tokens.reshape(row_count, local_width).astype(jnp.float32)
    scaled = (inputs * mix_gain).astype(jnp.bfloat16)
    forget_rows = lax.dynamic_slice_in_dim(w_forget, kv_index * local_width, local_width, 0)
    forget_cols = lax.dynamic_slice_in_dim(forget_rows, tp_index * heads_dev, heads_dev, 1)
    query_part = jnp.dot(scaled, w_query, preferred_element_type=jnp.float32)
    key_part = jnp.dot(scaled, w_key, preferred_element_type=jnp.float32)
    value_part = jnp.dot(scaled, w_value, preferred_element_type=jnp.float32)
    forget_part = jnp.dot(scaled, forget_cols, preferred_element_type=jnp.float32)
    squares = jnp.sum(inputs * inputs, axis=1)
    query_sum, key_sum, value_sum, forget_sum, square_sum = (
        lax.psum(query_part.astype(jnp.bfloat16), "kv").astype(jnp.float32),
        lax.psum(key_part.astype(jnp.bfloat16), "kv").astype(jnp.float32),
        lax.psum(value_part.astype(jnp.bfloat16), "kv").astype(jnp.float32),
        lax.psum(forget_part.astype(jnp.bfloat16), "kv").astype(jnp.float32),
        lax.psum(squares.astype(jnp.bfloat16), "kv").astype(jnp.float32),
    )
    inv_norm = lax.rsqrt(square_sum / D + EPSILON)[:, None]
    head_shape = (seq_count, new_count, heads_dev, head_width)
    query = (inv_norm * query_sum).astype(jnp.bfloat16).reshape(head_shape)
    key_new = (inv_norm * key_sum).astype(jnp.bfloat16).reshape(head_shape)
    value_new = (inv_norm * value_sum).astype(jnp.bfloat16).reshape(head_shape)
    log_forget = jax.nn.log_sigmoid(inv_norm * forget_sum + forget_bias).reshape(
        seq_count, new_count, heads_dev
    )
    score_scale = head_width ** (-0.5)
    positions = kv_index * pos_dev + jnp.arange(pos_dev, dtype=jnp.int32)
    live_rows = positions[None, :] < lengths[:, None]
    live_mask = live_rows[:, None, None, :]
    cached_keys = key_cache.reshape(seq_count, pos_dev, heads_dev, head_width)
    cached_values = value_cache.reshape(seq_count, pos_dev, heads_dev, head_width)
    scores = jnp.einsum("bthd,bphd->bthp", query, cached_keys, preferred_element_type=jnp.float32)
    scores = scores * score_scale - cum_gate[:, None]
    scores = jnp.where(live_mask, scores, NEG_FILL)
    block_peak = jnp.max(scores, axis=3)
    weights = jnp.where(live_mask, jnp.exp(scores - block_peak[..., None]), 0.0)
    block_total = jnp.sum(weights, axis=3)
    block_sum = jnp.einsum(
        "bthp,bphd->bthd",
        weights.astype(jnp.bfloat16),
        cached_values,
        preferred_element_type=jnp.float32,
    )
    last_hit = positions[None, :] == (lengths - 1)[:, None]
    last_piece = jnp.sum(jnp.where(last_hit[:, None, :], cum_gate, 0.0), axis=2)

    def combine(first, second):
        peak_both = jnp.maximum(first[0], second[0])
        first_factor = jnp.exp(first[0] - peak_both)
        second_factor = jnp.exp(second[0] - peak_both)
        return (
            peak_both,
            first[1] * first_factor + second[1] * second_factor,
            first[2] * first_factor[..., None] + second[2] * second_factor[..., None],
            first[3] + second[3],
        )

    past_peak, past_total, past_sum, last_cum = combined_all(
        (block_peak, block_total, block_sum, last_piece), "kv", combine
    )
    key_cum = last_cum[:, None, :] + jnp.cumsum(log_forget, axis=1)
    own_scores = (
        jnp.einsum("bthd,bshd->bths", query, key_new, preferred_element_type=jnp.float32)
        * score_scale
    )
    own_scores = own_scores - jnp.transpose(key_cum, (0, 2, 1))[:, None]
    causal = (jnp.arange(new_count)[:, None] >= jnp.arange(new_count)[None, :])[None, :, None, :]
    own_scores = jnp.where(causal, own_scores, NEG_FILL)
    peak_score = jnp.maximum(past_peak, jnp.max(own_scores, axis=3))
    past_factor = jnp.exp(past_peak - peak_score)
    own_weights = jnp.where(causal, jnp.exp(own_scores - peak_score[..., None]), 0.0)
    numerator = past_sum * past_factor[..., None] + jnp.einsum(
        "bths,bshd->bthd",
        own_weights.astype(jnp.bfloat16),
        value_new,
        preferred_element_type=jnp.float32,
    )
    denominator = past_total * past_factor + jnp.sum(own_weights, axis=3)
    attended = (
        (numerator / denominator[..., None])
        .astype(jnp.bfloat16)
        .reshape(row_count, heads_dev * head_width)
    )
    attn_out = lax.psum(
        jnp.dot(attended, w_out, preferred_element_type=jnp.float32).astype(jnp.bfloat16), "tp"
    ).astype(jnp.float32)
    middle = (inputs + attn_out).astype(jnp.bfloat16)
    middle_wide = middle.astype(jnp.float32)
    squares2 = jnp.sum(middle_wide * middle_wide, axis=1)
    scaled2 = (middle_wide * mlp_gain).astype(jnp.bfloat16)
    gate_part = jnp.dot(scaled2, w_gate, preferred_element_type=jnp.float32)
    up_part = jnp.dot(scaled2, w_up, preferred_element_type=jnp.float32)
    gate_sum, up_sum, square_sum2 = (
        lax.psum(gate_part.astype(jnp.bfloat16), "kv").astype(jnp.float32),
        lax.psum(up_part.astype(jnp.bfloat16), "kv").astype(jnp.float32),
        lax.psum(squares2.astype(jnp.bfloat16), "kv").astype(jnp.float32),
    )
    inv_norm2 = lax.rsqrt(square_sum2 / D + EPSILON)[:, None]
    hidden = (jax.nn.silu(inv_norm2 * gate_sum) * (inv_norm2 * up_sum)).astype(jnp.bfloat16)
    down_part = jnp.dot(hidden, w_down, preferred_element_type=jnp.float32)
    mixed = lax.psum(down_part.astype(jnp.bfloat16), "tp").astype(jnp.float32)
    return (middle_wide + mixed).astype(jnp.bfloat16).reshape(seq_count, new_count, local_width)


LANES = 128
MESH = pl.DeviceIdType.MESH
F32 = jnp.float32
BF16 = jnp.bfloat16


def fused_kernel(
    n_kv, n_tp, new_count,
    tok_h, mix_gain, mlp_gain, bias, lens, wf_h, cum_h, wq_h, wk_h, wv_h,
    kc_h, vc_h, wo_h, wg_h, wu_h, wd_h,
    out,
    wf, cum, wq, wk, wv, kc, vc, wo, wg, wu, wd,
    sb1, rb1, sb2, rb2, qb, inv_keep, lf, cs, cr, ab, ap, ar, mid, gs, gy, gf, gr, us, uy, uf, ur, ha, hb, dp, dr,
    lsem, ksem, vsem, s1, r1, s2, r2, s3, r3, s4, r4, s5, r5, s6, r6, s7, r7, s8, r8, s9, r9,
    s10, r10, s11, r11, s12, r12, s13, s14, r14, s15, tok, tok_blocks,
):
    me = lax.axis_index("kv")
    mt = lax.axis_index("tp")
    rows, width = tok.shape
    rp = rows // n_kv
    sp = rp // new_count
    heads = bias.shape[0]
    hw = wq.shape[1]
    hd = hw // heads
    pos_dev = kc.shape[1]
    ff = wg.shape[1]
    first_width = ha.shape[2]
    full = width * n_kv
    scale = hd ** (-0.5)

    pairs = n_kv // 2
    z, y = lax.div(me, 2), lax.rem(me, 2)
    mate = 2 * z + 1 - y

    def peer(i):
        return lax.rem(me + i, n_kv)

    def tpeer(i):
        return lax.rem(mt + i, n_tp)

    loads = [
        pltpu.make_async_copy(wf_h.at[:, pl.ds(pl.multiple_of(me * width, width), width)], wf, lsem.at[0]),
        pltpu.make_async_copy(wq_h, wq, lsem.at[1]),
        pltpu.make_async_copy(wk_h, wk, lsem.at[2]),
        pltpu.make_async_copy(wv_h, wv, lsem.at[3]),
        pltpu.make_async_copy(cum_h, cum, lsem.at[4]),
        pltpu.make_async_copy(wo_h, wo, lsem.at[5]),
        pltpu.make_async_copy(wg_h, wg, lsem.at[6]),
        pltpu.make_async_copy(wu_h, wu, lsem.at[7]),
        pltpu.make_async_copy(wd_h, wd, lsem.at[8]),
    ]

    def cache_copies(g):
        part = pl.ds(g * sp, sp)
        return (
            pltpu.make_async_copy(kc_h.at[part], kc.at[part], ksem.at[g]),
            pltpu.make_async_copy(vc_h.at[part], vc.at[part], vsem.at[g]),
        )

    tok_load = pltpu.make_async_copy(tok_h, tok_blocks, lsem.at[9])
    tok_load.start()
    for load in loads[:5]:
        load.start()

    def start_cache(i, c):
        for copy in cache_copies(peer(i)):
            copy.start()
        return c

    lax.fori_loop(0, n_kv, start_cache, 0)
    for load in loads[5:]:
        load.start()

    barrier = pltpu.get_barrier_semaphore()
    for i in range(1, n_kv):
        pl.semaphore_signal(barrier, inc=1, device_id={"kv": peer(i)}, device_id_type=MESH)
    for i in range(1, n_tp):
        pl.semaphore_signal(barrier, inc=1, device_id={"tp": tpeer(i)}, device_id_type=MESH)

    def send_kv(src, dst, send, recv, g):
        return pltpu.make_async_remote_copy(
            src_ref=src, dst_ref=dst, send_sem=send, recv_sem=recv,
            device_id={"kv": g}, device_id_type=MESH,
        )

    def send_tp(src, dst, send, recv, g):
        return pltpu.make_async_remote_copy(
            src_ref=src, dst_ref=dst, send_sem=send, recv_sem=recv,
            device_id={"tp": g}, device_id_type=MESH,
        )

    tok_load.wait()
    for b in range(tok_blocks.shape[0]):
        tok[b * new_count : (b + 1) * new_count] = tok_blocks[b].astype(F32)
    inputs = tok[...]
    scaled = (inputs * mix_gain[...]).astype(BF16)
    squares = jnp.sum(inputs * inputs, axis=1, keepdims=True)
    loads[0].wait()
    forget_all = lax.dot_general(
        scaled, wf[...], (((1,), (1,)), ((), ())), preferred_element_type=F32
    ).astype(BF16)
    pick_row = lax.broadcasted_iota(jnp.int32, (wf.shape[0], LANES), 0)
    pick_col = lax.broadcasted_iota(jnp.int32, (wf.shape[0], LANES), 1)
    pick = jnp.where(
        (pick_row == pick_col + mt * heads) & (pick_col < heads), 1.0, 0.0
    ).astype(BF16)
    forget = jnp.dot(forget_all, pick, preferred_element_type=F32)
    lane_rows = lax.broadcasted_iota(jnp.int32, (rows, LANES), 1)
    aux = jnp.where(lane_rows == heads, squares, forget)
    for g in range(n_kv):
        sb1[g, :, hw:] = aux[g * rp : (g + 1) * rp].astype(BF16)

    def project(load, weight, dest, first):
        load.wait()
        part = jnp.dot(scaled, weight[...], preferred_element_type=F32)
        for g in range(n_kv):
            dest[g, :, first : first + hw] = part[g * rp : (g + 1) * rp].astype(BF16)

    project(loads[1], wq, sb1, 0)
    pl.semaphore_wait(barrier, n_kv + n_tp - 2)
    for i in range(1, n_kv):
        g = peer(i)
        send_kv(sb1.at[g], rb1.at[me], s1.at[g], r1.at[me], g).start()
    project(loads[2], wk, sb2, 0)
    project(loads[3], wv, sb2, hw)
    total1 = sb1[me].astype(F32)
    for i in range(1, n_kv):
        g = peer(i)
        send_kv(sb1.at[g], rb1.at[g], s1.at[g], r1.at[g], g).wait_recv()
        total1 = total1 + rb1[g].astype(F32)
    lane = lax.broadcasted_iota(jnp.int32, (rp, LANES), 1)
    row8 = lax.broadcasted_iota(jnp.int32, (rp, LANES), 0)
    aux1 = total1[:, hw:]
    inv_norm = lax.rsqrt(aux1[:, heads : heads + 1] / full + EPSILON)
    qb[me] = (inv_norm * total1[:, :hw]).astype(BF16)
    for i in range(1, n_kv):
        g = peer(i)
        send_kv(qb.at[me], qb.at[me], s2.at[g], r2.at[me], g).start()
    for i in range(1, n_kv):
        g = peer(i)
        send_kv(sb2.at[g], rb2.at[me], s10.at[g], r10.at[me], g).start()
    bias_row = jnp.zeros((rp, LANES), F32)
    for h in range(heads):
        bias_row = jnp.where(lane == h, bias[h], bias_row)
    logit = inv_norm * aux1 + bias_row
    lf[...] = -(jnp.maximum(-logit, 0.0) + jnp.log1p(jnp.exp(-jnp.abs(logit))))
    inv_keep[...] = jnp.broadcast_to(inv_norm, (rp, LANES))

    loads[4].wait()
    col_q = lax.broadcasted_iota(jnp.int32, (rp, hw), 1)
    row_p = lax.broadcasted_iota(jnp.int32, (rp, pos_dev), 0)
    pos = me * pos_dev + lax.broadcasted_iota(jnp.int32, (rp, pos_dev), 1)

    def attend(g, dest):
        q8 = qb[g].astype(F32)
        spread = jnp.concatenate(
            [
                jnp.where((col_q >= h * hd) & (col_q < (h + 1) * hd), q8, 0.0)
                for h in range(heads)
            ],
            axis=0,
        ).astype(BF16)
        copy_k, copy_v = cache_copies(g)
        copy_k.wait()
        length = jnp.zeros((rp, pos_dev), jnp.int32)
        products, gates = [], []
        for j in range(sp):
            products.append(
                lax.dot_general(
                    spread, kc[g * sp + j], (((1,), (1,)), ((), ())), preferred_element_type=F32
                )
            )
            gates.append(cum[g * sp + j])
            length = jnp.where(row_p >= j * new_count, lens[g * sp + j], length)
        live = pos < length
        last_hit = pos == length - 1
        weight_heads = []
        extra = jnp.zeros((rp, LANES), F32)
        for h in range(heads):
            score, gate = None, None
            for j in range(sp):
                score_j = products[j][h * rp : (h + 1) * rp]
                gate_j = jnp.broadcast_to(gates[j][h : h + 1], (rp, pos_dev))
                if j == 0:
                    score, gate = score_j, gate_j
                else:
                    score = jnp.where(row_p >= j * new_count, score_j, score)
                    gate = jnp.where(row_p >= j * new_count, gate_j, gate)
            score = jnp.where(live, score * scale - gate, NEG_FILL)
            peak = jnp.max(score, axis=1, keepdims=True)
            weight = jnp.where(live, jnp.exp(score - peak), 0.0)
            extra = jnp.where(lane == h, peak, extra)
            extra = jnp.where(lane == heads + h, jnp.sum(weight, axis=1, keepdims=True), extra)
            last = jnp.sum(jnp.where(last_hit, gate, 0.0), axis=1, keepdims=True)
            extra = jnp.where(lane == 2 * heads + h, last, extra)
            weight_heads.append(weight)
        weights = jnp.concatenate(weight_heads, axis=0).astype(BF16)
        copy_v.wait()
        sums = [
            jnp.dot(weights, vc[g * sp + j], preferred_element_type=F32) for j in range(sp)
        ]
        row_h = row8[:, :1]
        for h in range(heads):
            piece = sums[0][h * rp : (h + 1) * rp, h * hd : (h + 1) * hd]
            for j in range(1, sp):
                piece_j = sums[j][h * rp : (h + 1) * rp, h * hd : (h + 1) * hd]
                piece = jnp.where(row_h >= j * new_count, piece_j, piece)
            dest[:, h * hd : (h + 1) * hd] = piece
        dest[:, hw:] = extra

    attend(me, cr.at[me])

    def attend_step(i, c):
        g = peer(i)
        send_kv(qb.at[me], qb.at[g], s2.at[g], r2.at[g], g).wait_recv()
        attend(g, cs.at[g])
        send_kv(cs.at[g], cr.at[me], s3.at[g], r3.at[me], g).start()
        return c

    lax.fori_loop(1, n_kv, attend_step, 0)

    total2 = sb2[me].astype(F32)
    for i in range(1, n_kv):
        g = peer(i)
        send_kv(sb2.at[g], rb2.at[g], s10.at[g], r10.at[g], g).wait_recv()
        total2 = total2 + rb2[g].astype(F32)
    own_scale = inv_keep[:, :1]
    own_key = (own_scale * total2[:, :hw]).astype(BF16).astype(F32)
    own_value = (own_scale * total2[:, hw:]).astype(BF16).astype(F32)
    for i in range(1, n_kv):
        g = peer(i)
        send_kv(cs.at[g], cr.at[g], s3.at[g], r3.at[g], g).wait_recv()

    def expand(x):
        return jnp.concatenate(
            [jnp.broadcast_to(x[:, h : h + 1], (rp, hd)) for h in range(heads)], axis=1
        )

    extras = [cr[k, :, hw:] for k in range(n_kv)]
    past_peak = functools.reduce(jnp.maximum, extras)
    past_total = jnp.zeros((rp, LANES), F32)
    last_cum = jnp.zeros((rp, LANES), F32)
    past_sum = jnp.zeros((rp, hw), F32)
    for k in range(n_kv):
        factor = jnp.exp(extras[k] - past_peak)
        past_total = past_total + pltpu.roll(extras[k], LANES - heads, 1) * factor
        last_cum = last_cum + pltpu.roll(extras[k], LANES - 2 * heads, 1)
        past_sum = past_sum + cr[k, :, :hw] * expand(factor)

    def valid(d):
        hit = (row8 >= d) & (row8 < new_count)
        for j in range(1, sp):
            hit = hit | ((row8 >= j * new_count + d) & (row8 < (j + 1) * new_count))
        return hit

    def shifted(x, d):
        return x if d == 0 else pltpu.roll(x, d, 0)

    log_forget = lf[...]
    key_cum = last_cum
    for d in range(new_count):
        key_cum = key_cum + jnp.where(valid(d), shifted(log_forget, d), 0.0)
    own_query = qb[me].astype(F32)
    own_scores = []
    for d in range(new_count):
        product = own_query * shifted(own_key, d)
        score = jnp.zeros((rp, LANES), F32)
        for h in range(heads):
            dot_h = jnp.sum(product[:, h * hd : (h + 1) * hd], axis=1, keepdims=True)
            score = jnp.where(lane == h, dot_h, score)
        own_scores.append(
            jnp.where(valid(d), score * scale - shifted(key_cum, d), NEG_FILL)
        )
    peak_score = functools.reduce(jnp.maximum, own_scores, past_peak)
    past_factor = jnp.exp(past_peak - peak_score)
    numerator = past_sum * expand(past_factor)
    denominator = past_total * past_factor
    for d in range(new_count):
        own_weight = jnp.where(valid(d), jnp.exp(own_scores[d] - peak_score), 0.0)
        denominator = denominator + own_weight
        numerator = numerator + expand(own_weight.astype(BF16).astype(F32)) * shifted(own_value, d)
    ab[me] = (numerator / expand(denominator)).astype(BF16)
    for i in range(1, n_kv):
        g = peer(i)
        send_kv(ab.at[me], ab.at[me], s4.at[g], r4.at[me], g).start()
    for i in range(1, n_kv):
        g = peer(i)
        send_kv(ab.at[me], ab.at[g], s4.at[g], r4.at[g], g).wait_recv()

    def all_rows(ref):
        return jnp.concatenate([ref[k].astype(F32) for k in range(n_kv)], axis=0).astype(BF16)

    loads[5].wait()
    ap[...] = jnp.dot(all_rows(ab), wo[...], preferred_element_type=F32).astype(BF16)
    for i in range(1, n_tp):
        g = tpeer(i)
        send_tp(ap, ar.at[mt], s5.at[g], r5.at[mt], g).start()
    for i in range(1, n_tp):
        g = tpeer(i)
        send_tp(ap, ar.at[g], s5.at[g], r5.at[g], g).wait_recv()
    attn_out = jnp.zeros((rows, width), F32)
    for k in range(n_tp):
        attn_out = attn_out + jnp.where(mt == k, ap[...], ar[k]).astype(F32)
    middle = (tok[...] + attn_out).astype(BF16)
    mid[...] = middle
    wide = middle.astype(F32)
    squares2 = jnp.sum(wide * wide, axis=1, keepdims=True)
    scaled2 = (wide * mlp_gain[...]).astype(BF16)

    for g in range(n_kv):
        gs[g, :, 2 * first_width :] = jnp.broadcast_to(
            squares2[g * rp : (g + 1) * rp], (rp, LANES)
        ).astype(BF16)
    tile = 256 if ff % 256 == 0 and first_width % 256 == 0 else LANES
    loads[6].wait()
    loads[7].wait()
    for start, span, sent, landed, ssem, rsem in (
        (0, first_width, gs, gy, s6, r6),
        (first_width, ff - first_width, us, uy, s7, r7),
    ):
        for offset, weight in ((0, wg), (span, wu)):

            def column_tile(
                c, carry, start=start, offset=offset, weight=weight, sent=sent
            ):
                cols = pl.ds(pl.multiple_of(start + c * tile, tile), tile)
                part = jnp.dot(scaled2, weight[:, cols], preferred_element_type=F32)
                place = pl.ds(pl.multiple_of(offset + c * tile, tile), tile)
                for g in range(n_kv):
                    sent[g, :, place] = part[g * rp : (g + 1) * rp].astype(BF16)
                return carry

            lax.fori_loop(0, span // tile, column_tile, 0)
        for i in range(1, pairs + 1):
            zz = lax.rem(z + i, pairs)
            send_kv(sent.at[2 * zz + 1 - y], landed.at[zz], ssem.at[zz], rsem.at[zz], mate).start()

    def second_hop(sent, landed, forward, arrived, ssem, rsem, ssem2, rsem2):
        for i in range(1, pairs + 1):
            zz = lax.rem(z + i, pairs)
            send_kv(sent.at[2 * zz + 1 - y], landed.at[zz], ssem.at[zz], rsem.at[zz], mate).wait_recv()
            both = sent[2 * zz + y].astype(F32) + landed[zz].astype(F32)
            if i == pairs:
                return both
            forward[zz] = both.astype(BF16)
            send_kv(
                forward.at[zz], arrived.at[z], ssem2.at[zz], rsem2.at[z], 2 * zz + y
            ).start()

    def finish_sum(both, forward, arrived, ssem2, rsem2):
        for i in range(1, pairs):
            zz = lax.rem(z + i, pairs)
            send_kv(
                forward.at[zz], arrived.at[zz], ssem2.at[zz], rsem2.at[zz], 2 * zz + y
            ).wait_recv()
            both = both + arrived[zz].astype(F32)
        return both

    def gather_start(block, ssem, msem, rsem):
        for i in range(1, pairs):
            zz = lax.rem(z + i, pairs)
            send_kv(block.at[me], block.at[me], ssem.at[zz], rsem.at[me], 2 * zz + y).start()
        send_kv(block.at[me], block.at[me], msem.at[z], rsem.at[me], mate).start()

    def gather_forward(block, ssem, msem, rsem):
        for i in range(1, pairs):
            zz = lax.rem(z + i, pairs)
            slot = 2 * zz + y
            send_kv(block.at[me], block.at[slot], ssem.at[zz], rsem.at[slot], slot).wait_recv()
            send_kv(block.at[slot], block.at[slot], msem.at[zz], rsem.at[slot], mate).start()

    def gather_end(block, msem, rsem):
        for i in range(1, pairs + 1):
            zz = lax.rem(z + i, pairs)
            slot = 2 * zz + 1 - y
            send_kv(block.at[me], block.at[slot], msem.at[zz], rsem.at[slot], mate).wait_recv()

    def gated(total, span):
        gate = inv_norm2 * total[:, :span]
        return (gate / (1.0 + jnp.exp(-gate)) * (inv_norm2 * total[:, span : 2 * span])).astype(BF16)

    first_both = second_hop(gs, gy, gf, gr, s6, r6, s11, r11)
    second_both = second_hop(us, uy, uf, ur, s7, r7, s12, r12)
    first_sum = finish_sum(first_both, gf, gr, s11, r11)
    inv_norm2 = lax.rsqrt(
        first_sum[:, 2 * first_width : 2 * first_width + 1] / full + EPSILON
    )
    ha[me] = gated(first_sum, first_width)
    gather_start(ha, s8, s13, r8)
    second_sum = finish_sum(second_both, uf, ur, s12, r12)
    hb[me] = gated(second_sum, ff - first_width)
    gather_start(hb, s14, s15, r14)
    gather_forward(ha, s8, s13, r8)
    gather_forward(hb, s14, s15, r14)
    gather_end(ha, s13, r8)

    loads[8].wait()
    down = jnp.dot(all_rows(ha), wd[:first_width], preferred_element_type=F32)
    gather_end(hb, s15, r14)
    down = down + jnp.dot(all_rows(hb), wd[first_width:], preferred_element_type=F32)
    dp[...] = down.astype(BF16)
    for i in range(1, n_tp):
        g = tpeer(i)
        send_tp(dp, dr.at[mt], s9.at[g], r9.at[mt], g).start()
    for i in range(1, n_tp):
        g = tpeer(i)
        send_tp(dp, dr.at[g], s9.at[g], r9.at[g], g).wait_recv()
    mixed = jnp.zeros((rows, width), F32)
    for k in range(n_tp):
        mixed = mixed + jnp.where(mt == k, dp[...], dr[k]).astype(F32)
    out[...] = (mid[...].astype(F32) + mixed).astype(BF16)

    for i in range(1, n_kv):
        g = peer(i)
        send_kv(sb1.at[g], rb1.at[me], s1.at[g], r1.at[me], g).wait_send()
        send_kv(qb.at[me], qb.at[me], s2.at[g], r2.at[me], g).wait_send()
        send_kv(cs.at[g], cr.at[me], s3.at[g], r3.at[me], g).wait_send()
        send_kv(ab.at[me], ab.at[me], s4.at[g], r4.at[me], g).wait_send()
        send_kv(sb2.at[g], rb2.at[me], s10.at[g], r10.at[me], g).wait_send()
    for zz in range(pairs):
        send_kv(gs.at[0], gy.at[zz], s6.at[zz], r6.at[zz], mate).wait_send()
        send_kv(us.at[0], uy.at[zz], s7.at[zz], r7.at[zz], mate).wait_send()
        send_kv(ha.at[me], ha.at[me], s13.at[zz], r8.at[me], mate).wait_send()
        send_kv(hb.at[me], hb.at[me], s15.at[zz], r14.at[me], mate).wait_send()
    for i in range(1, pairs):
        zz = lax.rem(z + i, pairs)
        g = 2 * zz + y
        send_kv(gf.at[zz], gr.at[z], s11.at[zz], r11.at[z], g).wait_send()
        send_kv(uf.at[zz], ur.at[z], s12.at[zz], r12.at[z], g).wait_send()
        send_kv(ha.at[me], ha.at[me], s8.at[zz], r8.at[me], g).wait_send()
        send_kv(hb.at[me], hb.at[me], s14.at[zz], r14.at[me], g).wait_send()
    for i in range(1, n_tp):
        g = tpeer(i)
        send_tp(ap, ar.at[mt], s5.at[g], r5.at[mt], g).wait_send()
        send_tp(dp, dr.at[mt], s9.at[g], r9.at[mt], g).wait_send()


def fused_on_device(
    tokens, mix_gain, w_query, w_key, w_value, w_forget, forget_bias, key_cache, value_cache,
    cum_gate, lengths, w_out, mlp_gain, w_gate, w_up, w_down,
):
    n_kv, n_tp = lax.axis_size("kv"), lax.axis_size("tp")
    seq_count, new_count, width = tokens.shape
    rows = seq_count * new_count
    rp = rows // n_kv
    hw = w_query.shape[1]
    ff = w_gate.shape[1]
    first_width = -(-ff // 512) * 256
    vmem = pl.BlockSpec(memory_space=pltpu.VMEM)
    smem = pl.BlockSpec(memory_space=pltpu.SMEM)
    anywhere = pl.BlockSpec(memory_space=pl.ANY)
    kv_sems = pltpu.SemaphoreType.DMA((n_kv,))
    tp_sems = pltpu.SemaphoreType.DMA((n_tp,))

    def like(x):
        return pltpu.VMEM(x.shape, x.dtype)

    result = pl.pallas_call(
        functools.partial(fused_kernel, n_kv, n_tp, new_count),
        out_shape=jax.ShapeDtypeStruct((rows, width), BF16),
        in_specs=[anywhere] + [vmem] * 2 + [smem] * 2 + [anywhere] * 11,
        out_specs=vmem,
        scratch_shapes=[
            pltpu.VMEM((w_forget.shape[1], width), BF16),
            like(cum_gate), like(w_query), like(w_key), like(w_value),
            like(key_cache), like(value_cache), like(w_out), like(w_gate), like(w_up),
            like(w_down),
            pltpu.VMEM((n_kv, rp, hw + LANES), BF16),
            pltpu.VMEM((n_kv, rp, hw + LANES), BF16),
            pltpu.VMEM((n_kv, rp, 2 * hw), BF16),
            pltpu.VMEM((n_kv, rp, 2 * hw), BF16),
            pltpu.VMEM((n_kv, rp, hw), BF16),
            pltpu.VMEM((rp, LANES), F32),
            pltpu.VMEM((rp, LANES), F32),
            pltpu.VMEM((n_kv, rp, hw + LANES), F32),
            pltpu.VMEM((n_kv, rp, hw + LANES), F32),
            pltpu.VMEM((n_kv, rp, hw), BF16),
            pltpu.VMEM((rows, width), BF16),
            pltpu.VMEM((n_tp, rows, width), BF16),
            pltpu.VMEM((rows, width), BF16),
            pltpu.VMEM((n_kv, rp, 2 * first_width + LANES), BF16),
            pltpu.VMEM((n_kv // 2, rp, 2 * first_width + LANES), BF16),
            pltpu.VMEM((n_kv // 2, rp, 2 * first_width + LANES), BF16),
            pltpu.VMEM((n_kv // 2, rp, 2 * first_width + LANES), BF16),
            pltpu.VMEM((n_kv, rp, 2 * (ff - first_width)), BF16),
            pltpu.VMEM((n_kv // 2, rp, 2 * (ff - first_width)), BF16),
            pltpu.VMEM((n_kv // 2, rp, 2 * (ff - first_width)), BF16),
            pltpu.VMEM((n_kv // 2, rp, 2 * (ff - first_width)), BF16),
            pltpu.VMEM((n_kv, rp, first_width), BF16),
            pltpu.VMEM((n_kv, rp, ff - first_width), BF16),
            pltpu.VMEM((rows, width), BF16),
            pltpu.VMEM((n_tp, rows, width), BF16),
            pltpu.SemaphoreType.DMA((10,)),
            kv_sems, kv_sems,
            kv_sems, kv_sems, kv_sems, kv_sems, kv_sems, kv_sems, kv_sems, kv_sems,
            tp_sems, tp_sems,
            kv_sems, kv_sems, kv_sems, kv_sems, kv_sems, kv_sems,
            tp_sems, tp_sems,
            kv_sems, kv_sems, kv_sems, kv_sems, kv_sems, kv_sems, kv_sems,
            kv_sems, kv_sems, kv_sems,
            pltpu.VMEM((rows, width), F32),
            like(tokens),
        ],
        compiler_params=pltpu.CompilerParams(
            collective_id=0, has_side_effects=True, vmem_limit_bytes=60 * 1024 * 1024
        ),
    )(
        tokens, mix_gain.reshape(1, width), mlp_gain.reshape(1, width),
        forget_bias, lengths, w_forget.T, cum_gate, w_query, w_key, w_value,
        key_cache, value_cache, w_out, w_gate, w_up, w_down,
    )
    return result.reshape(seq_count, new_count, width)


def solution(mesh):
    in_specs = (
        P(None, None, "kv"),
        P("kv"),
        P("kv", "tp"),
        P("kv", "tp"),
        P("kv", "tp"),
        P(),
        P("tp"),
        P(None, "kv", "tp"),
        P(None, "kv", "tp"),
        P(None, "tp", "kv"),
        P(),
        P("tp", "kv"),
        P("kv"),
        P("kv", "tp"),
        P("kv", "tp"),
        P("tp", "kv"),
    )
    out_specs = P(None, None, "kv")

    def layer(*arrays):
        seq_count, new_count, _ = arrays[0].shape
        rows_kv, rest = divmod(seq_count * new_count, jax.lax.axis_size("kv"))
        if rest or rows_kv % 8 or rows_kv % new_count or jax.lax.axis_size("kv") % 2:
            return on_device(*arrays)
        return fused_on_device(*arrays)

    return jax.shard_map(
        layer, mesh=mesh, in_specs=in_specs, out_specs=out_specs, check_vma=False
    )
```
